256 devices in a mesh: grp: 2 (over y), sp: 32 (over z, core), tp: 4 (over x).
Axes of the slice: x: 4, y: 2, z: 16, core: 2. Of those that a mesh axis runs over, the one named last changes fastest.
The devices are a block of a 4x16x16 slice.
Arguments:
- mix_in: bfloat16 [16384, 1536], P(('grp', 'sp'), 'tp'), parts along dimension 0, may hold values from -6 to 6
- resid_in: bfloat16 [16384, 2048], P(('grp', 'sp', 'tp')), parts along dimension 0, may hold values from -6 to 6
- doc_ids: int32 [16384], P(('grp', 'sp')), parts along dimension 0, may hold values from 0 to 15, never falling along the last dimension, each value on 1 to 768 neighbouring positions
- group_weight: bfloat16 [4, 384, 384], P('tp'), may hold values from -0.3125 to 0.3125
- pool_scale: float32 [1536], P('tp'), may hold values from 0.1 to 1.9
- out_weight: bfloat16 [1536, 2048], P('tp'), may hold values from -0.15625 to 0.15625
- norm_gain: float32 [2048], replicated, may hold values from 0.1 to 1.9
- expert_ids: int32 [16384, 2], P(('grp', 'sp', 'tp')), parts along dimension 0, may hold values from 0 to 127, as said below
- route_weights: float32 [16384, 2], P(('grp', 'sp', 'tp')), parts along dimension 0, may hold values from 0.1 to 1
- w_gate: bfloat16 [128, 2048, 512], P(('sp', 'tp')), may hold values from -0.125 to 0.125
- w_up: bfloat16 [128, 2048, 512], P(('sp', 'tp')), may hold values from -0.125 to 0.125
- w_down: bfloat16 [128, 512, 2048], P(('sp', 'tp')), may hold values from -0.25 to 0.25
Outputs:
- layer_out: bfloat16 [16384, 2048], P(('grp', 'sp', 'tp')), parts along dimension 0
The draws below stay inside these ranges and needn't reach their ends.
There are 2 independent parts, one for each index of `grp`. The reference program is written for one: setup_inputs(seed, part) draws one part's arguments, and reference() takes and returns one part's arrays. A program takes and returns all parts, laid end to end along the dimension named above; an argument that names none is the same for every part. Nothing has to cross between parts.
Inputs may be any that keep to these rules, and one draw needn't show every extreme that they name: `doc_ids`: document numbers never fall along the positions. `expert_ids`: each row names two different experts of one group of 32 consecutive experts. Among the rows of one device (aligned blocks of 64 rows) no expert is named more than 2 times; in every draw the experts of some group are each named exactly 2 times in every block.
All inputs are finite; a program needn't handle non-finite values.
Results may differ from the reference program's by a relative error of at most 0.012.
Values may be sent and summed in bfloat16 or wider, within the bound.
A program may use at most 64 MiB of HBM per device.

```python
import math
import jax
import jax.numpy as jnp
import numpy as np
from jax import lax

D = 2048
GD = 384
FF = 512
POOL_GROUPS = 4
HALO = 16
EXPERT_GROUPS = 4
TOP_K = 2
MIX = 1536
SLICE = 64
TOKENS = 8192
EXPERTS = 128
EPG = 32
CAP = 2
DOCS = 16
SEG_MOST = 768


def block_order(subkey):
    return jax.random.permutation(subkey, SLICE)


def draw_expert_ids(key, part):
    blocks = TOKENS // SLICE
    busy_count = EPG * CAP // 2
    subkeys = jax.random.split(jax.random.fold_in(key, 11), 5)
    busy_group = jax.random.randint(subkeys[0], (), 0, EXPERT_GROUPS)
    spare_pick = jax.random.randint(subkeys[1], (blocks, SLICE), 0, EXPERT_GROUPS - 1)
    position = jnp.arange(SLICE, dtype=jnp.int32)[None, :]
    unshuffled = jnp.where(position < busy_count, busy_group, (busy_group + 1 + spare_pick) % EXPERT_GROUPS)
    row_order = jax.vmap(block_order)(jax.random.split(subkeys[2], blocks))
    row_group = jnp.take_along_axis(unshuffled, row_order, axis=1)
    onehot = (row_group[:, :, None] == jnp.arange(EXPERT_GROUPS, dtype=jnp.int32)[None, None, :]).astype(jnp.int32)
    row_rank = jnp.sum(onehot * (jnp.cumsum(onehot, axis=1) - 1), axis=2)
    first_shift = jax.random.randint(subkeys[3], (blocks, EXPERT_GROUPS), 0, EPG)
    second_shift = jax.random.randint(subkeys[4], (blocks, EXPERT_GROUPS), 0, EPG - 1)
    first_base = jnp.take_along_axis(first_shift, row_group, axis=1)
    second_extra = jnp.take_along_axis(second_shift, row_group, axis=1)
    first_pick = row_group * EPG + (row_rank + first_base) % EPG
    second_pick = row_group * EPG + (row_rank + first_base + 1 + second_extra) % EPG
    return jnp.stack([first_pick, second_pick], axis=-1).reshape(TOKENS, TOP_K).astype(jnp.int32)


def block_scale(stream_key, dims, shards, low, largest):
    level, own = 1.0, jax.random.fold_in(stream_key, 6)
    for dim, shards_of in shards:
        heights = jnp.exp(jax.random.uniform(jax.random.fold_in(own, dim), (shards_of,), jnp.float32, low / len(shards), largest / len(shards)))
        level = level * jnp.repeat(heights, dims[dim] // shards_of).reshape([-1 if axis == dim else 1 for axis in range(len(dims))])
    return level


def length_profile(number_of, total, most, skew):
    portions = [(1 << 20) // math.isqrt(rank ** skew) + 1 for rank in range(2, number_of + 1)]
    rest, holding = total - most - (number_of - 1), [1] * (number_of - 1)
    while rest > 0:
        candidates = [i for i in range(number_of - 1) if holding[i] < most]
        whole, budget = sum([portions[i] for i in candidates]), rest
        for i in candidates:
            extra = min(most - holding[i], max(1, budget * portions[i] // whole), rest)
            holding[i] = holding[i] + extra
            rest = rest - extra
    return np.array([most] + holding)


def ragged(own_key, amount, total, most, slope):
    if amount == 2:
        one = jax.random.randint(own_key, (), max(1, total - most), min(most, total - 1) + 1)
        return jnp.stack([one, total - one])
    tallies = jnp.asarray(length_profile(amount, total, most, slope), jnp.int32)
    pairs = (amount - 1) // 2
    source_of, sink = tallies[1:1 + 2 * pairs:2], tallies[2:2 + 2 * pairs:2]
    margin = jnp.minimum(source_of - 1, most - sink)
    moved = jax.random.randint(jax.random.fold_in(own_key, 1), (pairs,), 0, 1 << 20) % (margin + 1)
    tallies = tallies.at[1:1 + 2 * pairs:2].set(source_of - moved).at[2:2 + 2 * pairs:2].set(sink + moved)
    return tallies[jax.random.permutation(jax.random.fold_in(own_key, 2), amount)]


def scatter_about(stream_key, dims, deviation, most, cuts=(), kind=jnp.bfloat16):
    loudness = block_scale(stream_key, dims, cuts, -0.22, 0.18) if cuts else 1.0
    entries = jax.random.normal(stream_key, dims, jnp.float32) * deviation * loudness
    return jnp.minimum(jnp.maximum(entries, -most), most).astype(kind)


def setup_inputs(seed: int = 0, part: int = 0) -> dict:
    keys = jax.random.split(jax.random.key(seed), 13)
    part_splits = jax.random.split(jax.random.fold_in(keys[12], part), 13)
    return {
        "mix_in": scatter_about(part_splits[0], (TOKENS, MIX), 1.0, 6.0, ((0, 32), (1, 4))),
        "resid_in": scatter_about(part_splits[1], (TOKENS, D), 1.0, 6.0, ((0, 128),)),
        "doc_ids": jnp.searchsorted(jnp.cumsum(ragged(part_splits[2], DOCS, TOKENS, SEG_MOST, 2)), jnp.arange(TOKENS), side="right").astype(jnp.int32),
        "group_weight": scatter_about(keys[3], (POOL_GROUPS, GD, GD), GD ** -0.5, 0.3125, ((0, 4),)),
        "pool_scale": jnp.clip(1.0 + 0.18 * jax.random.normal(keys[4], (MIX,), jnp.float32), 0.1, 1.9),
        "out_weight": scatter_about(keys[5], (MIX, D), MIX ** -0.5, 0.15625, ((0, 4),)),
        "norm_gain": jnp.clip(1.0 + 0.18 * jax.random.normal(keys[6], (D,), jnp.float32), 0.1, 1.9),
        "expert_ids": draw_expert_ids(jax.random.fold_in(jax.random.fold_in(keys[12], part), 71), part),
        "route_weights": jnp.clip(jnp.exp(math.log(1.0) - 2.3025851 * jax.random.uniform(part_splits[8], (TOKENS, TOP_K), jnp.float32) ** block_scale(part_splits[8], (TOKENS, TOP_K), ((0, 128),), -0.2, 0.2)), 0.1, 1.0),
        "w_gate": scatter_about(keys[9], (EXPERTS, D, FF), D ** -0.5, 0.125, ((0, 128),)),
        "w_up": scatter_about(keys[10], (EXPERTS, D, FF), D ** -0.5, 0.125, ((0, 128),)),
        "w_down": scatter_about(keys[11], (EXPERTS, FF, D), FF ** -0.5, 0.25, ((0, 128),)),
    }


def expert_rows(flat_rows, gate_matrix, up_matrix, down_matrix):
    gate_part = jnp.dot(flat_rows, gate_matrix, preferred_element_type=jnp.float32)
    up_part = jnp.dot(flat_rows, up_matrix, preferred_element_type=jnp.float32)
    hidden = (jax.nn.silu(gate_part) * up_part).astype(jnp.bfloat16)
    return jnp.dot(hidden, down_matrix, preferred_element_type=jnp.float32).astype(jnp.bfloat16)

def reference(mix_in, resid_in, doc_ids, group_weight, pool_scale, out_weight, norm_gain, expert_ids, route_weights, w_gate, w_up, w_down):
    marked = doc_ids.astype(jnp.int32) + 1
    padded = jnp.concatenate([jnp.zeros((HALO, MIX), jnp.float32), mix_in.astype(jnp.float32)], axis=0)
    pad_marks = jnp.concatenate([jnp.zeros((HALO,), jnp.int32), marked])
    reach = jnp.left_shift(jnp.int32(2), jnp.arange(MIX, dtype=jnp.int32) // GD)
    running = jnp.zeros((TOKENS, MIX), jnp.float32)
    members = jnp.zeros((TOKENS, MIX), jnp.float32)
    for offset in range(HALO):
        rows_back = padded[HALO - offset:HALO - offset + TOKENS]
        same_doc = pad_marks[HALO - offset:HALO - offset + TOKENS] == marked
        keep = same_doc[:, None] & (offset < reach)[None, :]
        running = running + jnp.where(keep, rows_back, 0.0)
        members = members + keep.astype(jnp.float32)
    mixed = (running / members - mix_in.astype(jnp.float32)).astype(jnp.bfloat16)
    pieces = []
    for group_index in range(POOL_GROUPS):
        lower = group_index * GD
        product = jnp.dot(mixed[:, lower:lower + GD], group_weight[group_index], preferred_element_type=jnp.float32)
        pieces.append((product * pool_scale[lower:lower + GD]).astype(jnp.bfloat16))
    grouped = jnp.concatenate(pieces, axis=1)
    projected = jnp.dot(grouped, out_weight, preferred_element_type=jnp.float32)
    stream = (resid_in.astype(jnp.float32) + projected).astype(jnp.bfloat16)
    stream_f = stream.astype(jnp.float32)
    level = lax.optimization_barrier(jnp.mean(stream_f * stream_f, axis=1, keepdims=True))
    normed = (stream_f * lax.rsqrt(level + 1e-06) * norm_gain.astype(jnp.float32)).astype(jnp.bfloat16)
    route_total = TOKENS * TOP_K
    route_expert = expert_ids.reshape(-1).astype(jnp.int32)
    onehot = (route_expert[:, None] == jnp.arange(EXPERTS, dtype=jnp.int32)[None, :]).astype(jnp.int32)
    slot_index = lax.optimization_barrier(jnp.sum(onehot * (jnp.cumsum(onehot, axis=0) - 1), axis=1)).astype(jnp.int32)
    table = jnp.full((EXPERTS, EXPERTS * CAP), route_total, jnp.int32)
    table = table.at[route_expert, slot_index].set(jnp.arange(route_total, dtype=jnp.int32))
    normed_pad = jnp.concatenate([normed, jnp.zeros((1, D), jnp.bfloat16)], axis=0)

    def serve(answers, inputs):
        gate_matrix, up_matrix, down_matrix, routes = inputs
        rows_in = normed_pad[routes // TOP_K]
        served = expert_rows(rows_in, gate_matrix, up_matrix, down_matrix)
        return (answers.at[routes].set(served), None)
    answers, _ = lax.scan(serve, jnp.zeros((route_total + 1, D), jnp.bfloat16), (w_gate, w_up, w_down, table))
    weighted = answers[:route_total].astype(jnp.float32) * route_weights.reshape(-1)[:, None]
    paired = weighted.reshape(TOKENS, TOP_K, D)
    return (stream_f + paired[:, 0] + paired[:, 1]).astype(jnp.bfloat16)
```

```python
import jax
import jax.numpy as jnp
from jax import lax
from jax.experimental import pallas as pl
from jax.experimental.pallas import tpu as pltpu
from jax.sharding import PartitionSpec as P

MESH = pl.DeviceIdType.MESH
BF = jnp.bfloat16
F32 = jnp.float32
HALO = 16
EPG = 32
CAP = 2
NB = 4


def dot(a, b):
    return lax.dot_general(a, b, (((1,), (0,)), ((), ())), preferred_element_type=F32)


def dot_t(a, b):
    return lax.dot_general(a, b, (((0,), (0,)), ((), ())), preferred_element_type=F32)


def iota(shape, dim):
    return lax.broadcasted_iota(jnp.int32, shape, dim)


def drain(ref, sem):
    pltpu.make_async_copy(ref, ref, sem).wait()


def kernel(
    sp_size,
    tp_size,
    mix_hbm,
    resid_hbm,
    doc_ref,
    gw_hbm,
    scale_ref,
    ow_hbm,
    gain_ref,
    ids_ref,
    rw_ref,
    wg_hbm,
    wu_hbm,
    wd_hbm,
    out_ref,
    mix_v,
    halo_v,
    hdoc_v,
    resid_v,
    gw_v,
    ow_v,
    wg_v,
    wu_v,
    wd_v,
    mixed_v,
    grouped_v,
    s1_out,
    s1_in,
    s2_out,
    s2_in,
    stream_v,
    a_out,
    m_out,
    a_in,
    m_in,
    b_out,
    b_in,
    r_out,
    r_in,
    c_out,
    c_in,
    load_sem,
    halo_sem,
    s_send,
    s_recv,
    a_send,
    a_recv,
    b_send,
    b_recv,
    r_send,
    r_recv,
    c_send,
    c_recv,
):
    sp, tp = lax.axis_index("sp"), lax.axis_index("tp")
    rows, width = mix_v.shape
    mine, model = stream_v.shape
    half = model // 2
    cols = model // NB
    slots = a_out.shape[1] // NB
    block_sp = EPG // tp_size
    depth = block_sp // 2
    blocks = sp_size // block_sp

    chip, core = sp // 2, lax.rem(sp, 2)
    block, place = chip // depth, lax.rem(chip, depth)
    local = lax.rem(sp, block_sp) * tp_size + tp

    def at(chip_at):
        return {"sp": chip_at * 2 + core, "tp": tp}

    def peer(k):
        other = lax.rem(local + k, EPG)
        return other, {"sp": block * block_sp + other // tp_size, "tp": lax.rem(other, tp_size)}

    low = place < 2
    mod = lax.rem(place, 2)

    def of_block(step, place_at):
        return lax.rem(block + step, blocks) * depth + place_at

    relays = {
        1: (of_block(1, jnp.where(low, 1, 0)), mod),
        2: (of_block(2, jnp.where(low, place + 2, place - 2)), jnp.int32(2)),
        3: (of_block(3, jnp.where(low, 3, 2)), mod),
    }
    side = jnp.where(low, blocks - 1, 1)
    first = jnp.where(mod == 0, 2, 0)
    sources = [
        (of_block(side, first), jnp.where(low, 1, 3)),
        (of_block(side, first + 1), jnp.where(low, 1, 3)),
        (of_block(2, jnp.where(low, place + 2, place - 2)), jnp.int32(2)),
    ]
    after, before = lax.rem(sp + 1, sp_size), lax.rem(sp + sp_size - 1, sp_size)
    right, left = lax.rem(tp + 1, tp_size), lax.rem(tp + tp_size - 1, tp_size)

    def remote(src, dst, send, recv, where):
        return pltpu.make_async_remote_copy(
            src_ref=src, dst_ref=dst, send_sem=send, recv_sem=recv, device_id=where, device_id_type=MESH
        )

    barrier = pltpu.get_barrier_semaphore()

    def greet(where):
        pl.semaphore_signal(barrier, inc=1, device_id=where, device_id_type=MESH)

    for step in (1, 2, 3):
        greet(at(relays[step][0]))
    for source, _ in sources:
        greet(at(source))
    greet({"sp": before, "tp": tp})

    def greet_peer(k, carry):
        greet(peer(k)[1])
        return carry

    lax.fori_loop(1, EPG, greet_peer, 0)

    loads = [
        pltpu.make_async_copy(src, dst, load_sem.at[i])
        for i, (src, dst) in enumerate(
            (
                (mix_hbm, mix_v),
                (gw_hbm.at[0], gw_v),
                (ow_hbm, ow_v),
                (resid_hbm, resid_v),
                (wg_hbm.at[0], wg_v),
                (wu_hbm.at[0], wu_v),
                (wd_hbm.at[0], wd_v),
            )
        )
    ]
    for load in loads:
        load.start()

    first_id, second_id = ids_ref[:, 0:1], ids_ref[:, 1:2]
    lane = iota((mine, 128), 1)
    named_first, named_second = first_id == lane, second_id == lane
    earlier = (iota((mine, mine), 0) > iota((mine, mine), 1)).astype(BF)
    ahead = dot(earlier, (named_first | named_second).astype(BF))
    group = lax.shift_right_logical(first_id, EPG.bit_length() - 1)
    in_group = group == lane
    ahead_group = dot(earlier, in_group.astype(BF))
    rank = jnp.sum(jnp.where(in_group, ahead_group, 0.0), axis=1, keepdims=True).astype(jnp.int32)

    def row_of(ids, named):
        order = jnp.sum(jnp.where(named, ahead, 0.0), axis=1, keepdims=True)
        return (ids - group * EPG).astype(F32) * CAP + order + 1.0

    def thirds(value):
        top = value.astype(BF).astype(F32)
        middle = (value - top).astype(BF).astype(F32)
        return [top, middle, value - top - middle]

    entries = [row_of(first_id, named_first), row_of(second_id, named_second)]
    entries += thirds(rw_ref[:, 0:1]) + thirds(rw_ref[:, 1:2])
    table = jnp.zeros((mine, 128), F32)
    for i, entry in enumerate(entries):
        table = jnp.where(lane == i, entry, table)
    table = table.astype(BF)
    step_of = lax.rem(group - block + blocks, blocks)
    chosen = (step_of * slots + rank == lane).astype(BF)
    for step in range(blocks):
        picked = ((step_of == step) & (rank == lax.rem(lane, slots))).astype(BF)
        m_out[step] = dot_t(table, picked)[0:8]

    loads[0].wait()
    reach = jnp.left_shift(jnp.int32(2), tp)
    doc_row = doc_ref[...]
    sub, lan = iota((rows, rows), 0), iota((rows, rows), 1)
    doc_col = jnp.sum(jnp.where(sub == lan, doc_row, 0).astype(F32), axis=1, keepdims=True)
    doc_row = doc_row.astype(F32)
    member = (doc_col == doc_row) & (sub >= lan) & (sub - lan < reach)
    member = member.astype(F32)
    count = jnp.sum(member, axis=1, keepdims=True)
    total = dot(member.astype(BF), mix_v[...])
    mixed_v[...] = (total / count - mix_v[...].astype(F32)).astype(BF)
    tail = halo_v.shape[0] - HALO
    halo_v[0:tail] = jnp.zeros((tail, width), BF)

    pl.semaphore_wait(barrier, EPG - 1 + 3 + 3 + 1)
    next_dev = {"sp": after, "tp": tp}
    halo = [
        remote(mix_v.at[pl.ds(rows - HALO, HALO)], halo_v.at[pl.ds(tail, HALO)], halo_sem.at[0], halo_sem.at[1], next_dev),
        remote(doc_ref, hdoc_v, halo_sem.at[2], halo_sem.at[3], next_dev),
    ]
    for copy in halo:
        copy.start()
    for copy in halo:
        copy.wait_recv()
    hdoc = hdoc_v[:, rows - 128 :].astype(F32)
    hsub, hlan = iota((HALO, 128), 0), iota((HALO, 128), 1)
    hmember = (doc_col[0:HALO] == hdoc) & (hsub + 128 - hlan < reach) & (sp > 0)
    hmember = hmember.astype(F32)
    hcount = count[0:HALO] + jnp.sum(hmember, axis=1, keepdims=True)
    htotal = total[0:HALO] + dot(hmember.astype(BF), halo_v[...])
    mixed_v[0:HALO] = (htotal / hcount - mix_v[0:HALO].astype(F32)).astype(BF)

    loads[1].wait()
    grouped_v[...] = (dot(mixed_v[...], gw_v[...]) * scale_ref[...]).astype(BF)
    loads[2].wait()

    def part(owner, lo, n):
        piece = grouped_v[pl.ds(pl.multiple_of(owner * mine, mine), mine)]
        return dot(piece, ow_v[:, lo : lo + n])

    opposite = lax.rem(tp + 2, tp_size)
    to_right, to_left = {"sp": sp, "tp": right}, {"sp": sp, "tp": left}
    hops = []
    for i, where in enumerate((to_right, to_left)):
        s1_out[i] = part(opposite, i * half, half).astype(BF)
        copy = remote(s1_out.at[i], s1_in.at[i], s_send.at[i], s_recv.at[i], where)
        copy.start()
        hops.append(copy)
    for i, (owner, where) in enumerate(((right, to_right), (left, to_left))):
        j = 1 - i
        s2_out[i, j] = part(owner, j * half, half).astype(BF)
        copy = remote(s2_out.at[i, j], s2_in.at[i, j], s_send.at[2 + 2 * i + j], s_recv.at[2 + 2 * i + j], where)
        copy.start()
        hops.append(copy)
    sums = [part(right, 0, half), part(left, half, half)]
    for i, where in enumerate((to_right, to_left)):
        hops[i].wait_recv()
        s2_out[i, i] = (sums[i] + s1_in[i].astype(F32)).astype(BF)
        copy = remote(s2_out.at[i, i], s2_in.at[i, i], s_send.at[2 + 3 * i], s_recv.at[2 + 3 * i], where)
        copy.start()
        hops.append(copy)
    own = [part(tp, 0, half), part(tp, half, half)]
    loads[3].wait()
    for copy in hops[2:]:
        copy.wait_recv()
    level = jnp.zeros((mine, 1), F32)
    streams = []
    for j in range(2):
        projected = own[j] + s2_in[0, j].astype(F32) + s2_in[1, j].astype(F32)
        stream = (resid_v[:, j * half : (j + 1) * half].astype(F32) + projected).astype(BF)
        stream_v[:, j * half : (j + 1) * half] = stream
        stream = stream.astype(F32)
        level += jnp.sum(stream * stream, axis=1, keepdims=True)
        streams.append(stream)
    factor = lax.rsqrt(level / model + 1e-06)
    for j in range(2):
        normed = (streams[j] * factor * gain_ref[:, j * half : (j + 1) * half]).astype(BF)
        packed = dot_t(chosen, normed).astype(BF)
        for b in range(NB // 2):
            at_row = (j * (NB // 2) + b) * slots
            for step in range(blocks):
                a_out[step, at_row : at_row + slots] = packed[
                    step * slots : (step + 1) * slots, b * cols : (b + 1) * cols
                ]
    forwards = []
    for step in (1, 3, 2):
        chip_at, slot = relays[step]
        for src, dst, n in ((m_out, m_in, 0), (a_out, a_in, 1)):
            copy = remote(src.at[step], dst.at[slot], a_send.at[step - 1, n], a_recv.at[slot, n], at(chip_at))
            copy.start()
            forwards.append(copy)

    line = iota((EPG * CAP * NB, 128), 0).astype(F32)
    block_of = (iota((1, 128), 1) // slots).astype(F32)

    def hits(meta):
        spots = []
        for i in range(2):
            entry = meta[i : i + 1]
            spots.append(line == jnp.where(entry > 0.0, (entry - 1.0) * NB + block_of, -1.0))
        return spots

    def send_rows(out, into, send, recv, q):
        into[q, local] = out[q, local]

        def one(k, carry):
            other, where = peer(k)
            remote(out.at[q, other], into.at[q, local], send.at[q], recv.at[q], where).start()
            return carry

        lax.fori_loop(1, EPG, one, 0)

    def relay(meta, tokens, q):
        one, two = hits(meta)
        sent = dot((one | two).astype(BF), tokens).astype(BF)
        b_out[q] = sent.reshape(EPG, CAP * NB, cols)
        send_rows(b_out, b_in, b_send, b_recv, q)

    def combine(meta, q):
        drain(r_in.at[q, pl.ds(0, EPG - 1)], r_recv.at[q])
        one, two = hits(meta)
        weigh = [meta[2 + 3 * i : 3 + 3 * i] + meta[3 + 3 * i : 4 + 3 * i] + meta[4 + 3 * i : 5 + 3 * i] for i in range(2)]
        weights = jnp.where(one, weigh[0], 0.0) + jnp.where(two, weigh[1], 0.0)
        high = weights.astype(BF)
        rest = (weights - high.astype(F32)).astype(BF)
        answers = r_in[q].reshape(EPG * CAP * NB, cols)
        return (dot_t(high, answers) + dot_t(rest, answers)).astype(BF)

    many = EPG * CAP
    turn_r, turn_c = iota((many * NB, many * NB), 0), iota((many * NB, many * NB), 1)
    to_blocks = (lax.rem(turn_r, many) * NB + turn_r // many == turn_c).astype(BF)
    to_rows = (lax.rem(turn_c, many) * NB + turn_c // many == turn_r).astype(BF)

    def serve(q):
        drain(b_in.at[q, pl.ds(0, EPG - 1)], b_recv.at[q])
        x = dot(to_blocks, b_in[q].reshape(many * NB, cols)).astype(BF)
        gate = jnp.zeros((many, wg_v.shape[1]), F32)
        up = jnp.zeros((many, wg_v.shape[1]), F32)
        for b in range(NB):
            xb = x[b * many : (b + 1) * many]
            gate += dot(xb, wg_v[b * cols : (b + 1) * cols])
            up += dot(xb, wu_v[b * cols : (b + 1) * cols])
        hidden = (gate * jax.nn.sigmoid(gate) * up).astype(BF)
        answers = [dot(hidden, wd_v[:, b * cols : (b + 1) * cols]).astype(BF) for b in range(NB)]
        served = dot(to_rows, jnp.concatenate(answers, axis=0)).astype(BF)
        r_out[q] = served.reshape(EPG, CAP * NB, cols)
        send_rows(r_out, r_in, r_send, r_recv, q)

    relay(m_out[0], a_out[0], 0)
    for load in loads[4:]:
        load.wait()

    def back(slot):
        source, step = sources[slot]
        return remote(
            c_out.at[slot],
            c_in.at[:, pl.ds(pl.multiple_of(step * slots, slots), slots)],
            c_send.at[slot],
            c_recv.at[step],
            at(source),
        )

    def store_combined(q):
        if q == 0:
            c_in[:, 0:slots] = combine(m_out[0], 0).reshape(NB, slots, cols)
        else:
            c_out[q - 1] = combine(m_in[q - 1], q).reshape(NB, slots, cols)
            back(q - 1).start()

    for q in range(4):
        if q < 3:
            for n, ref in enumerate((m_in, a_in)):
                drain(ref.at[q], a_recv.at[q, n])
            relay(m_in[q], a_in[q], q + 1)
        serve(q)
        if q > 0:
            store_combined(q - 1)
    store_combined(3)

    for step in (1, 2, 3):
        drain(c_in.at[:, pl.ds(step * slots, slots)], c_recv.at[step])
    for b in range(NB):
        total = dot(chosen, c_in[b])
        span = slice(b * cols, (b + 1) * cols)
        out_ref[:, span] = (stream_v[:, span].astype(F32) + total).astype(BF)

    for copy in halo + hops + forwards:
        copy.wait_send()
    for q in range(4):
        drain(b_out.at[q, pl.ds(0, EPG - 1)], b_send.at[q])
        drain(r_out.at[q, pl.ds(0, EPG - 1)], r_send.at[q])
    for slot in range(3):
        back(slot).wait_send()


def shards(mix_in, resid_in, doc_ids, group_weight, pool_scale, out_weight, norm_gain, expert_ids, route_weights, w_gate, w_up, w_down):
    sp_size, tp_size = lax.axis_size("sp"), lax.axis_size("tp")
    rows, width = mix_in.shape
    mine, model = resid_in.shape
    hidden = w_gate.shape[2]
    cols = model // NB
    slots = mine // 2
    steps = sp_size * tp_size // EPG
    anywhere, vmem = pl.BlockSpec(memory_space=pl.ANY), pl.BlockSpec(memory_space=pltpu.VMEM)
    dma = pltpu.SemaphoreType.DMA
    message = (4, EPG, CAP * NB, cols)

    def body(*refs):
        kernel(sp_size, tp_size, *refs)

    return pl.pallas_call(
        body,
        out_shape=jax.ShapeDtypeStruct((mine, model), BF),
        in_specs=[anywhere, anywhere, vmem, anywhere, vmem, anywhere, vmem, vmem, vmem, anywhere, anywhere, anywhere],
        out_specs=vmem,
        scratch_shapes=[
            pltpu.VMEM((rows, width), BF),
            pltpu.VMEM((128, width), BF),
            pltpu.VMEM((1, rows), jnp.int32),
            pltpu.VMEM((mine, model), BF),
            pltpu.VMEM((width, width), BF),
            pltpu.VMEM((width, model), BF),
            pltpu.VMEM((model, hidden), BF),
            pltpu.VMEM((model, hidden), BF),
            pltpu.VMEM((hidden, model), BF),
            pltpu.VMEM((rows, width), BF),
            pltpu.VMEM((rows, width), BF),
            pltpu.VMEM((2, mine, model // 2), BF),
            pltpu.VMEM((2, mine, model // 2), BF),
            pltpu.VMEM((2, 2, mine, model // 2), BF),
            pltpu.VMEM((2, 2, mine, model // 2), BF),
            pltpu.VMEM((mine, model), BF),
            pltpu.VMEM((steps, NB * slots, cols), BF),
            pltpu.VMEM((steps, 8, 128), F32),
            pltpu.VMEM((steps - 1, NB * slots, cols), BF),
            pltpu.VMEM((steps - 1, 8, 128), F32),
            pltpu.VMEM(message, BF),
            pltpu.VMEM(message, BF),
            pltpu.VMEM(message, BF),
            pltpu.VMEM(message, BF),
            pltpu.VMEM((steps - 1, NB, slots, cols), BF),
            pltpu.VMEM((NB, steps * slots, cols), BF),
            dma((7,)),
            dma((4,)),
            dma((6,)),
            dma((6,)),
            dma((3, 2)),
            dma((3, 2)),
            dma((4,)),
            dma((4,)),
            dma((4,)),
            dma((4,)),
            dma((3,)),
            dma((4,)),
        ],
        compiler_params=pltpu.CompilerParams(collective_id=0, has_side_effects=True, vmem_limit_bytes=60 * 1024 * 1024),
    )(
        mix_in,
        resid_in,
        doc_ids.reshape(1, rows),
        group_weight,
        pool_scale.reshape(1, width),
        out_weight,
        norm_gain.reshape(1, model),
        expert_ids,
        route_weights,
        w_gate,
        w_up,
        w_down,
    )


def solution(mesh):
    return jax.shard_map(
        shards,
        mesh=mesh,
        in_specs=(
            P(("grp", "sp"), "tp"),
            P(("grp", "sp", "tp"), None),
            P(("grp", "sp")),
            P("tp", None, None),
            P("tp"),
            P("tp", None),
            P(),
            P(("grp", "sp", "tp"), None),
            P(("grp", "sp", "tp"), None),
            P(("sp", "tp"), None, None),
            P(("sp", "tp"), None, None),
            P(("sp", "tp"), None, None),
        ),
        out_specs=P(("grp", "sp", "tp"), None),
        check_vma=False,
    )
```

```python
import jax
import jax.numpy as jnp
from jax import lax
from jax.experimental import pallas as pl
from jax.experimental.pallas import tpu as pltpu
from jax.sharding import PartitionSpec as P

MESH = pl.DeviceIdType.MESH
BF = jnp.bfloat16
F32 = jnp.float32
scope = jax.named_scope
HALO = 16
EPG = 32
CAP = 2
TOP_K = 2
SENDS = (1, 3, 2)
ORDER = "L0 L1 F0 X0 L2 F1 X1 C0 L3 F2 X2 C1 F3 X3 C2 C3".split()
NB = 4


def dot(a, b):
    return lax.dot_general(a, b, (((1,), (0,)), ((), ())), preferred_element_type=F32)


def dot_t(a, b):
    return lax.dot_general(a, b, (((0,), (0,)), ((), ())), preferred_element_type=F32)


def iota(shape, dim):
    return lax.broadcasted_iota(jnp.int32, shape, dim)


def drain(ref, sem):
    pltpu.make_async_copy(ref, ref, sem).wait()


def kernel(
    sp_size,
    tp_size,
    mix_hbm,
    resid_hbm,
    doc_ref,
    gw_hbm,
    scale_ref,
    ow_hbm,
    gain_ref,
    ids_ref,
    rw_ref,
    wg_hbm,
    wu_hbm,
    wd_hbm,
    out_ref,
    mix_v,
    halo_v,
    hdoc_v,
    resid_v,
    gw_v,
    ow_v,
    wg_v,
    wu_v,
    wd_v,
    mixed_v,
    grouped_v,
    s1_out,
    s1_in,
    s2_out,
    s2_in,
    stream_v,
    a_out,
    m_out,
    a_in,
    m_in,
    b_out,
    b_in,
    r_out,
    r_in,
    c_out,
    c_in,
    load_sem,
    halo_sem,
    s_send,
    s_recv,
    a_send,
    a_recv,
    b_send,
    b_recv,
    r_send,
    r_recv,
    c_send,
    c_recv,
):
    sp, tp = lax.axis_index("sp"), lax.axis_index("tp")
    rows, width = mix_v.shape
    mine, model = stream_v.shape
    half = model // 2
    cols = model // NB
    slots = a_out.shape[1] // NB
    block_sp = EPG // tp_size
    depth = block_sp // 2
    blocks = sp_size // block_sp

    chip, core = sp // 2, lax.rem(sp, 2)
    block, place = chip // depth, lax.rem(chip, depth)
    local = lax.rem(sp, block_sp) * tp_size + tp

    def at(chip_at):
        return {"sp": chip_at * 2 + core, "tp": tp}

    def peer(k):
        other = lax.rem(local + k, EPG)
        return other, {"sp": block * block_sp + other // tp_size, "tp": lax.rem(other, tp_size)}

    low = place < 2
    mod = lax.rem(place, 2)

    def of_block(step, place_at):
        return lax.rem(block + step, blocks) * depth + place_at

    relays = {
        1: (of_block(1, jnp.where(low, 1, 0)), mod),
        2: (of_block(2, jnp.where(low, place + 2, place - 2)), jnp.int32(2)),
        3: (of_block(3, jnp.where(low, 3, 2)), mod),
    }
    side = jnp.where(low, blocks - 1, 1)
    first = jnp.where(mod == 0, 2, 0)
    sources = [
        (of_block(side, first), jnp.where(low, 1, 3)),
        (of_block(side, first + 1), jnp.where(low, 1, 3)),
        (of_block(2, jnp.where(low, place + 2, place - 2)), jnp.int32(2)),
    ]
    after, before = lax.rem(sp + 1, sp_size), lax.rem(sp + sp_size - 1, sp_size)
    right, left = lax.rem(tp + 1, tp_size), lax.rem(tp + tp_size - 1, tp_size)

    def remote(src, dst, send, recv, where):
        return pltpu.make_async_remote_copy(
            src_ref=src, dst_ref=dst, send_sem=send, recv_sem=recv, device_id=where, device_id_type=MESH
        )

    barrier = pltpu.get_barrier_semaphore()

    def greet(where):
        pl.semaphore_signal(barrier, inc=1, device_id=where, device_id_type=MESH)

    for step in (1, 2, 3):
        greet(at(relays[step][0]))
    for source, _ in sources:
        greet(at(source))
    greet({"sp": before, "tp": tp})

    def greet_peer(k, carry):
        greet(peer(k)[1])
        return carry

    lax.fori_loop(1, EPG, greet_peer, 0)

    loads = [
        pltpu.make_async_copy(src, dst, load_sem.at[i])
        for i, (src, dst) in enumerate(
            (
                (mix_hbm, mix_v),
                (gw_hbm.at[0], gw_v),
                (ow_hbm, ow_v),
                (resid_hbm, resid_v),
                (wg_hbm.at[0], wg_v),
                (wu_hbm.at[0], wu_v),
                (wd_hbm.at[0], wd_v),
            )
        )
    ]
    for load in loads:
        load.start()

    same = iota((mine, mine), 0) == iota((mine, mine), 1)

    def column(row):
        return jnp.sum(jnp.where(same, row.astype(F32), 0.0), axis=1, keepdims=True)

    first_id, second_id = (column(ids_ref[i : i + 1]).astype(jnp.int32) for i in range(TOP_K))
    lane = iota((mine, 128), 1)
    named_first, named_second = first_id == lane, second_id == lane
    earlier = (iota((mine, mine), 0) > iota((mine, mine), 1)).astype(BF)
    ahead = dot(earlier, (named_first | named_second).astype(BF))
    group = lax.shift_right_logical(first_id, EPG.bit_length() - 1)
    in_group = group == lane
    ahead_group = dot(earlier, in_group.astype(BF))
    rank = jnp.sum(jnp.where(in_group, ahead_group, 0.0), axis=1, keepdims=True).astype(jnp.int32)

    def row_of(ids, named):
        order = jnp.sum(jnp.where(named, ahead, 0.0), axis=1, keepdims=True)
        return (ids - group * EPG).astype(F32) * CAP + order + 1.0

    def thirds(value):
        top = value.astype(BF).astype(F32)
        middle = (value - top).astype(BF).astype(F32)
        return [top, middle, value - top - middle]

    entries = [row_of(first_id, named_first), row_of(second_id, named_second)]
    entries += thirds(column(rw_ref[0:1])) + thirds(column(rw_ref[1:2]))
    table = jnp.zeros((mine, 128), F32)
    for i, entry in enumerate(entries):
        table = jnp.where(lane == i, entry, table)
    table = table.astype(BF)
    step_of = lax.rem(group - block + blocks, blocks)
    chosen = (step_of * slots + rank == lane).astype(BF)
    for step in range(blocks):
        picked = ((step_of == step) & (rank == lax.rem(lane, slots))).astype(BF)
        m_out[step] = dot_t(table, picked)[0:8]

    with scope("w_mix"):
        loads[0].wait()
    reach = jnp.left_shift(jnp.int32(2), tp)
    doc_row = doc_ref[...]
    sub, lan = iota((rows, rows), 0), iota((rows, rows), 1)
    doc_col = jnp.sum(jnp.where(sub == lan, doc_row, 0).astype(F32), axis=1, keepdims=True)
    doc_row = doc_row.astype(F32)
    member = (doc_col == doc_row) & (sub >= lan) & (sub - lan < reach)
    member = member.astype(F32)
    count = jnp.sum(member, axis=1, keepdims=True)
    total = dot(member.astype(BF), mix_v[...])
    mixed_v[...] = (total / count - mix_v[...].astype(F32)).astype(BF)
    tail = halo_v.shape[0] - HALO
    halo_v[0:tail] = jnp.zeros((tail, width), BF)

    with scope("w_bar"):
        pl.semaphore_wait(barrier, EPG - 1 + 3 + 3 + 1)
    next_dev = {"sp": after, "tp": tp}
    halo = [
        remote(mix_v.at[pl.ds(rows - HALO, HALO)], halo_v.at[pl.ds(tail, HALO)], halo_sem.at[0], halo_sem.at[1], next_dev),
        remote(doc_ref, hdoc_v, halo_sem.at[2], halo_sem.at[3], next_dev),
    ]
    for copy in halo:
        copy.start()
    with scope("w_halo"):
        for copy in halo:
            copy.wait_recv()
    hdoc = hdoc_v[:, rows - 128 :].astype(F32)
    hsub, hlan = iota((HALO, 128), 0), iota((HALO, 128), 1)
    hmember = (doc_col[0:HALO] == hdoc) & (hsub + 128 - hlan < reach) & (sp > 0)
    hmember = hmember.astype(F32)
    hcount = count[0:HALO] + jnp.sum(hmember, axis=1, keepdims=True)
    htotal = total[0:HALO] + dot(hmember.astype(BF), halo_v[...])
    mixed_v[0:HALO] = (htotal / hcount - mix_v[0:HALO].astype(F32)).astype(BF)

    with scope("w_gw"):
        loads[1].wait()
    grouped_v[...] = (dot(mixed_v[...], gw_v[...]) * scale_ref[...].reshape(1, width)).astype(BF)
    with scope("w_ow"):
        loads[2].wait()

    def part(owner, lo, n):
        piece = grouped_v[pl.ds(pl.multiple_of(owner * mine, mine), mine)]
        return dot(piece, ow_v[:, lo : lo + n])

    opposite = lax.rem(tp + 2, tp_size)
    to_right, to_left = {"sp": sp, "tp": right}, {"sp": sp, "tp": left}
    hops = []
    for i, where in enumerate((to_right, to_left)):
        s1_out[i] = part(opposite, i * half, half).astype(BF)
        copy = remote(s1_out.at[i], s1_in.at[i], s_send.at[i], s_recv.at[i], where)
        copy.start()
        hops.append(copy)
    for i, (owner, where) in enumerate(((right, to_right), (left, to_left))):
        j = 1 - i
        s2_out[i, j] = part(owner, j * half, half).astype(BF)
        copy = remote(s2_out.at[i, j], s2_in.at[i, j], s_send.at[2 + 2 * i + j], s_recv.at[2 + 2 * i + j], where)
        copy.start()
        hops.append(copy)
    sums = [part(right, 0, half), part(left, half, half)]
    for i, where in enumerate((to_right, to_left)):
        with scope(f"w_s1_{i}"):
            hops[i].wait_recv()
        s2_out[i, i] = (sums[i] + s1_in[i].astype(F32)).astype(BF)
        copy = remote(s2_out.at[i, i], s2_in.at[i, i], s_send.at[2 + 3 * i], s_recv.at[2 + 3 * i], where)
        copy.start()
        hops.append(copy)
    own = [part(tp, 0, half), part(tp, half, half)]
    with scope("w_s2"):
        loads[3].wait()
        for copy in hops[2:]:
            copy.wait_recv()
    level = jnp.zeros((mine, 1), F32)
    streams = []
    for j in range(2):
        projected = own[j] + s2_in[0, j].astype(F32) + s2_in[1, j].astype(F32)
        stream = (resid_v[:, j * half : (j + 1) * half].astype(F32) + projected).astype(BF)
        stream_v[:, j * half : (j + 1) * half] = stream
        stream = stream.astype(F32)
        level += jnp.sum(stream * stream, axis=1, keepdims=True)
        streams.append(stream)
    factor = lax.rsqrt(level / model + 1e-06)
    for j in range(2):
        normed = (streams[j] * factor * gain_ref[:, j * half : (j + 1) * half]).astype(BF)
        packed = dot_t(chosen, normed).astype(BF)
        for b in range(NB // 2):
            at_row = (j * (NB // 2) + b) * slots
            for step in range(blocks):
                a_out[step, at_row : at_row + slots] = packed[
                    step * slots : (step + 1) * slots, b * cols : (b + 1) * cols
                ]
    forwards = []
    for step in SENDS:
        chip_at, slot = relays[step]
        for src, dst, n in ((m_out, m_in, 0), (a_out, a_in, 1)):
            copy = remote(src.at[step], dst.at[slot], a_send.at[step - 1, n], a_recv.at[slot, n], at(chip_at))
            copy.start()
            forwards.append(copy)

    line = iota((EPG * CAP * NB, 128), 0).astype(F32)
    block_of = (iota((1, 128), 1) // slots).astype(F32)

    def hits(meta):
        spots = []
        for i in range(2):
            entry = meta[i : i + 1]
            spots.append(line == jnp.where(entry > 0.0, (entry - 1.0) * NB + block_of, -1.0))
        return spots

    def send_rows(out, into, send, recv, q):
        into[q, local] = out[q, local]

        def one(k, carry):
            other, where = peer(k)
            remote(out.at[q, other], into.at[q, local], send.at[q], recv.at[q], where).start()
            return carry

        lax.fori_loop(1, EPG, one, 0)

    def relay(meta, tokens, q):
        one, two = hits(meta)
        sent = dot((one | two).astype(BF), tokens).astype(BF)
        b_out[q] = sent.reshape(EPG, CAP * NB, cols)
        send_rows(b_out, b_in, b_send, b_recv, q)

    def combine(meta, q):
        with scope(f"w_r{q}"):
            drain(r_in.at[q, pl.ds(0, EPG - 1)], r_recv.at[q])
        one, two = hits(meta)
        weigh = [meta[2 + 3 * i : 3 + 3 * i] + meta[3 + 3 * i : 4 + 3 * i] + meta[4 + 3 * i : 5 + 3 * i] for i in range(2)]
        weights = jnp.where(one, weigh[0], 0.0) + jnp.where(two, weigh[1], 0.0)
        high = weights.astype(BF)
        rest = (weights - high.astype(F32)).astype(BF)
        answers = r_in[q].reshape(EPG * CAP * NB, cols)
        return (dot_t(high, answers) + dot_t(rest, answers)).astype(BF)

    many = EPG * CAP
    turn_r, turn_c = iota((many * NB, many * NB), 0), iota((many * NB, many * NB), 1)
    to_blocks = (lax.rem(turn_r, many) * NB + turn_r // many == turn_c).astype(BF)
    to_rows = (lax.rem(turn_c, many) * NB + turn_c // many == turn_r).astype(BF)

    def serve(q):
        with scope(f"w_b{q}"):
            drain(b_in.at[q, pl.ds(0, EPG - 1)], b_recv.at[q])
        x = dot(to_blocks, b_in[q].reshape(many * NB, cols)).astype(BF)
        gate = jnp.zeros((many, wg_v.shape[1]), F32)
        up = jnp.zeros((many, wg_v.shape[1]), F32)
        for b in range(NB):
            xb = x[b * many : (b + 1) * many]
            gate += dot(xb, wg_v[b * cols : (b + 1) * cols])
            up += dot(xb, wu_v[b * cols : (b + 1) * cols])
        hidden = (gate * jax.nn.sigmoid(gate) * up).astype(BF)
        answers = [dot(hidden, wd_v[:, b * cols : (b + 1) * cols]).astype(BF) for b in range(NB)]
        served = dot(to_rows, jnp.concatenate(answers, axis=0)).astype(BF)
        r_out[q] = served.reshape(EPG, CAP * NB, cols)

    def answer(q):
        send_rows(r_out, r_in, r_send, r_recv, q)

    def back(slot):
        source, step = sources[slot]
        return remote(
            c_out.at[slot],
            c_in.at[:, pl.ds(pl.multiple_of(step * slots, slots), slots)],
            c_send.at[slot],
            c_recv.at[step],
            at(source),
        )

    def store_combined(q):
        if q == 0:
            c_in[:, 0:slots] = combine(m_out[0], 0).reshape(NB, slots, cols)
        else:
            c_out[q - 1] = combine(m_in[q - 1], q).reshape(NB, slots, cols)
            back(q - 1).start()

    def pass_on(q):
        if q == 0:
            relay(m_out[0], a_out[0], 0)
        else:
            with scope(f"w_a{q}"):
                for n, ref in enumerate((m_in, a_in)):
                    drain(ref.at[q - 1], a_recv.at[q - 1, n])
            relay(m_in[q - 1], a_in[q - 1], q)

    acts = {"L": pass_on, "F": serve, "X": answer, "C": store_combined}
    for i, name in enumerate(ORDER):
        if i == 1:
            with scope("w_weights"):
                for load in loads[4:]:
                    load.wait()
        acts[name[0]](int(name[1]))

    for step in (1, 2, 3):
        with scope(f"w_c{step}"):
            drain(c_in.at[:, pl.ds(step * slots, slots)], c_recv.at[step])
    for b in range(NB):
        total = dot(chosen, c_in[b])
        span = slice(b * cols, (b + 1) * cols)
        out_ref[:, span] = (stream_v[:, span].astype(F32) + total).astype(BF)

    with scope("w_sends"):
        for copy in halo + hops + forwards:
            copy.wait_send()
        for q in range(4):
            drain(b_out.at[q, pl.ds(0, EPG - 1)], b_send.at[q])
            drain(r_out.at[q, pl.ds(0, EPG - 1)], r_send.at[q])
        for slot in range(3):
            back(slot).wait_send()


def shards(mix_in, resid_in, doc_ids, group_weight, pool_scale, out_weight, norm_gain, expert_ids, route_weights, w_gate, w_up, w_down):
    sp_size, tp_size = lax.axis_size("sp"), lax.axis_size("tp")
    rows, width = mix_in.shape
    mine, model = resid_in.shape
    hidden = w_gate.shape[2]
    cols = model // NB
    slots = mine // 2
    steps = sp_size * tp_size // EPG
    anywhere, vmem = pl.BlockSpec(memory_space=pl.ANY), pl.BlockSpec(memory_space=pltpu.VMEM)
    dma = pltpu.SemaphoreType.DMA
    message = (4, EPG, CAP * NB, cols)

    def body(*refs):
        kernel(sp_size, tp_size, *refs)

    return pl.pallas_call(
        body,
        out_shape=jax.ShapeDtypeStruct((mine, model), BF),
        in_specs=[anywhere, anywhere, vmem, anywhere, vmem, anywhere, vmem, vmem, vmem, anywhere, anywhere, anywhere],
        out_specs=vmem,
        scratch_shapes=[
            pltpu.VMEM((rows, width), BF),
            pltpu.VMEM((128, width), BF),
            pltpu.VMEM((1, rows), jnp.int32),
            pltpu.VMEM((mine, model), BF),
            pltpu.VMEM((width, width), BF),
            pltpu.VMEM((width, model), BF),
            pltpu.VMEM((model, hidden), BF),
            pltpu.VMEM((model, hidden), BF),
            pltpu.VMEM((hidden, model), BF),
            pltpu.VMEM((rows, width), BF),
            pltpu.VMEM((rows, width), BF),
            pltpu.VMEM((2, mine, model // 2), BF),
            pltpu.VMEM((2, mine, model // 2), BF),
            pltpu.VMEM((2, 2, mine, model // 2), BF),
            pltpu.VMEM((2, 2, mine, model // 2), BF),
            pltpu.VMEM((mine, model), BF),
            pltpu.VMEM((steps, NB * slots, cols), BF),
            pltpu.VMEM((steps, 8, 128), F32),
            pltpu.VMEM((steps - 1, NB * slots, cols), BF),
            pltpu.VMEM((steps - 1, 8, 128), F32),
            pltpu.VMEM(message, BF),
            pltpu.VMEM(message, BF),
            pltpu.VMEM(message, BF),
            pltpu.VMEM(message, BF),
            pltpu.VMEM((steps - 1, NB, slots, cols), BF),
            pltpu.VMEM((NB, steps * slots, cols), BF),
            dma((7,)),
            dma((4,)),
            dma((6,)),
            dma((6,)),
            dma((3, 2)),
            dma((3, 2)),
            dma((4,)),
            dma((4,)),
            dma((4,)),
            dma((4,)),
            dma((3,)),
            dma((4,)),
        ],
        compiler_params=pltpu.CompilerParams(collective_id=0, has_side_effects=True, vmem_limit_bytes=60 * 1024 * 1024),
    )(
        mix_in,
        resid_in,
        doc_ids.reshape(1, rows),
        group_weight,
        pool_scale,
        out_weight,
        norm_gain.reshape(1, model),
        expert_ids.T,
        route_weights.T,
        w_gate,
        w_up,
        w_down,
    )


def solution(mesh):
    return jax.shard_map(
        shards,
        mesh=mesh,
        in_specs=(
            P(("grp", "sp"), "tp"),
            P(("grp", "sp", "tp"), None),
            P(("grp", "sp")),
            P("tp", None, None),
            P("tp"),
            P("tp", None),
            P(),
            P(("grp", "sp", "tp"), None),
            P(("grp", "sp", "tp"), None),
            P(("sp", "tp"), None, None),
            P(("sp", "tp"), None, None),
            P(("sp", "tp"), None, None),
        ),
        out_specs=P(("grp", "sp", "tp"), None),
        check_vma=False,
    )
```

```python
import jax
import jax.numpy as jnp
from jax import lax
from jax.experimental import pallas as pl
from jax.experimental.pallas import tpu as pltpu
from jax.sharding import PartitionSpec as P

MESH = pl.DeviceIdType.MESH
BF = jnp.bfloat16
F32 = jnp.float32
scope = jax.named_scope
HALO = 16
EPG = 32
CAP = 2
TOP_K = 2
SENDS = (1, 3, 2)
ORDER = "L0 L1 F0 X0 L2 F1 X1 C0 L3 F2 X2 C1 F3 X3 C2 C3".split()
NB = 4


def dot(a, b):
    return lax.dot_general(a, b, (((1,), (0,)), ((), ())), preferred_element_type=F32)


def dot_t(a, b):
    return lax.dot_general(a, b, (((0,), (0,)), ((), ())), preferred_element_type=F32)


def iota(shape, dim):
    return lax.broadcasted_iota(jnp.int32, shape, dim)


def drain(ref, sem):
    pltpu.make_async_copy(ref, ref, sem).wait()


def kernel(
    sp_size,
    tp_size,
    mix_hbm,
    resid_hbm,
    doc_ref,
    gw_hbm,
    scale_ref,
    ow_hbm,
    gain_ref,
    ids_ref,
    rw_ref,
    wg_hbm,
    wu_hbm,
    wd_hbm,
    out_ref,
    mix_v,
    halo_v,
    hdoc_v,
    resid_v,
    gw_v,
    ow_v,
    wg_v,
    wu_v,
    wd_v,
    mixed_v,
    grouped_v,
    s1_out,
    s1_in,
    s2_out,
    s2_in,
    stream_v,
    a_out,
    m_out,
    a_in,
    m_in,
    b_out,
    b_in,
    r_out,
    r_in,
    c_out,
    c_in,
    load_sem,
    halo_sem,
    s_send,
    s_recv,
    a_send,
    a_recv,
    b_send,
    b_recv,
    r_send,
    r_recv,
    c_send,
    c_recv,
):
    sp, tp = lax.axis_index("sp"), lax.axis_index("tp")
    rows, width = mix_v.shape
    mine, model = stream_v.shape
    half = model // 2
    cols = model // NB
    slots = a_out.shape[1] // NB
    block_sp = EPG // tp_size
    depth = block_sp // 2
    blocks = sp_size // block_sp

    chip, core = sp // 2, lax.rem(sp, 2)
    block, place = chip // depth, lax.rem(chip, depth)
    local = lax.rem(sp, block_sp) * tp_size + tp

    def at(chip_at):
        return {"sp": chip_at * 2 + core, "tp": tp}

    def peer(k):
        other = lax.rem(local + k, EPG)
        return other, {"sp": block * block_sp + other // tp_size, "tp": lax.rem(other, tp_size)}

    low = place < 2
    mod = lax.rem(place, 2)

    def of_block(step, place_at):
        return lax.rem(block + step, blocks) * depth + place_at

    relays = {
        1: (of_block(1, jnp.where(low, 1, 0)), mod),
        2: (of_block(2, jnp.where(low, place + 2, place - 2)), jnp.int32(2)),
        3: (of_block(3, jnp.where(low, 3, 2)), mod),
    }
    side = jnp.where(low, blocks - 1, 1)
    first = jnp.where(mod == 0, 2, 0)
    sources = [
        (of_block(side, first), jnp.where(low, 1, 3)),
        (of_block(side, first + 1), jnp.where(low, 1, 3)),
        (of_block(2, jnp.where(low, place + 2, place - 2)), jnp.int32(2)),
    ]
    after, before = lax.rem(sp + 1, sp_size), lax.rem(sp + sp_size - 1, sp_size)
    right, left = lax.rem(tp + 1, tp_size), lax.rem(tp + tp_size - 1, tp_size)

    def remote(src, dst, send, recv, where):
        return pltpu.make_async_remote_copy(
            src_ref=src, dst_ref=dst, send_sem=send, recv_sem=recv, device_id=where, device_id_type=MESH
        )

    barrier = pltpu.get_barrier_semaphore()

    def greet(where):
        pl.semaphore_signal(barrier, inc=1, device_id=where, device_id_type=MESH)

    for step in (1, 2, 3):
        greet(at(relays[step][0]))
    for source, _ in sources:
        greet(at(source))
    greet({"sp": before, "tp": tp})

    def greet_peer(k, carry):
        greet(peer(k)[1])
        return carry

    lax.fori_loop(1, EPG, greet_peer, 0)

    loads = [
        pltpu.make_async_copy(src, dst, load_sem.at[i])
        for i, (src, dst) in enumerate(
            (
                (mix_hbm, mix_v),
                (gw_hbm.at[0], gw_v),
                (ow_hbm, ow_v),
                (resid_hbm, resid_v),
                (wg_hbm.at[0], wg_v),
                (wu_hbm.at[0], wu_v),
                (wd_hbm.at[0], wd_v),
            )
        )
    ]
    for load in loads:
        load.start()

    same = iota((mine, mine), 0) == iota((mine, mine), 1)

    def column(row):
        return jnp.sum(jnp.where(same, row.astype(F32), 0.0), axis=1, keepdims=True)

    first_id, second_id = (column(ids_ref[i : i + 1]).astype(jnp.int32) for i in range(TOP_K))
    lane = iota((mine, 128), 1)
    named_first, named_second = first_id == lane, second_id == lane
    earlier = (iota((mine, mine), 0) > iota((mine, mine), 1)).astype(BF)
    ahead = dot(earlier, (named_first | named_second).astype(BF))
    group = lax.shift_right_logical(first_id, EPG.bit_length() - 1)
    in_group = group == lane
    ahead_group = dot(earlier, in_group.astype(BF))
    rank = jnp.sum(jnp.where(in_group, ahead_group, 0.0), axis=1, keepdims=True).astype(jnp.int32)

    def row_of(ids, named):
        order = jnp.sum(jnp.where(named, ahead, 0.0), axis=1, keepdims=True)
        return (ids - group * EPG).astype(F32) * CAP + order + 1.0

    def thirds(value):
        top = value.astype(BF).astype(F32)
        middle = (value - top).astype(BF).astype(F32)
        return [top, middle, value - top - middle]

    entries = [row_of(first_id, named_first), row_of(second_id, named_second)]
    entries += thirds(column(rw_ref[0:1])) + thirds(column(rw_ref[1:2]))
    table = jnp.zeros((mine, 128), F32)
    for i, entry in enumerate(entries):
        table = jnp.where(lane == i, entry, table)
    table = table.astype(BF)
    step_of = lax.rem(group - block + blocks, blocks)
    chosen = (step_of * slots + rank == lane).astype(BF)
    for step in range(blocks):
        picked = ((step_of == step) & (rank == lax.rem(lane, slots))).astype(BF)
        m_out[step] = dot_t(table, picked)[0:8]

    with scope("w_mix"):
        loads[0].wait()
    reach = jnp.left_shift(jnp.int32(2), tp)
    doc_row = doc_ref[...]
    sub, lan = iota((rows, rows), 0), iota((rows, rows), 1)
    doc_col = jnp.sum(jnp.where(sub == lan, doc_row, 0).astype(F32), axis=1, keepdims=True)
    doc_row = doc_row.astype(F32)
    member = (doc_col == doc_row) & (sub >= lan) & (sub - lan < reach)
    member = member.astype(F32)
    count = jnp.sum(member, axis=1, keepdims=True)
    total = dot(member.astype(BF), mix_v[...])
    mixed_v[...] = (total / count - mix_v[...].astype(F32)).astype(BF)
    tail = halo_v.shape[0] - HALO
    halo_v[0:tail] = jnp.zeros((tail, width), BF)

    with scope("w_bar"):
        pl.semaphore_wait(barrier, EPG - 1 + 3 + 3 + 1)
    next_dev = {"sp": after, "tp": tp}
    halo = [
        remote(mix_v.at[pl.ds(rows - HALO, HALO)], halo_v.at[pl.ds(tail, HALO)], halo_sem.at[0], halo_sem.at[1], next_dev),
        remote(doc_ref, hdoc_v, halo_sem.at[2], halo_sem.at[3], next_dev),
    ]
    for copy in halo:
        copy.start()
    with scope("w_halo"):
        for copy in halo:
            copy.wait_recv()
    hdoc = hdoc_v[:, rows - 128 :].astype(F32)
    hsub, hlan = iota((HALO, 128), 0), iota((HALO, 128), 1)
    hmember = (doc_col[0:HALO] == hdoc) & (hsub + 128 - hlan < reach) & (sp > 0)
    hmember = hmember.astype(F32)
    hcount = count[0:HALO] + jnp.sum(hmember, axis=1, keepdims=True)
    htotal = total[0:HALO] + dot(hmember.astype(BF), halo_v[...])
    mixed_v[0:HALO] = (htotal / hcount - mix_v[0:HALO].astype(F32)).astype(BF)

    with scope("w_gw"):
        loads[1].wait()
    grouped_v[...] = (dot(mixed_v[...], gw_v[...]) * scale_ref[...].reshape(1, width)).astype(BF)
    with scope("w_ow"):
        loads[2].wait()

    def part(owner, lo, n):
        piece = grouped_v[pl.ds(pl.multiple_of(owner * mine, mine), mine)]
        return dot(piece, ow_v[:, lo : lo + n])

    opposite = lax.rem(tp + 2, tp_size)
    to_right, to_left = {"sp": sp, "tp": right}, {"sp": sp, "tp": left}
    hops = []
    for i, where in enumerate((to_right, to_left)):
        s1_out[i] = part(opposite, i * half, half).astype(BF)
        copy = remote(s1_out.at[i], s1_in.at[i], s_send.at[i], s_recv.at[i], where)
        copy.start()
        hops.append(copy)
    for i, (owner, where) in enumerate(((right, to_right), (left, to_left))):
        j = 1 - i
        s2_out[i, j] = part(owner, j * half, half).astype(BF)
        copy = remote(s2_out.at[i, j], s2_in.at[i, j], s_send.at[2 + 2 * i + j], s_recv.at[2 + 2 * i + j], where)
        copy.start()
        hops.append(copy)
    sums = [part(right, 0, half), part(left, half, half)]
    for i, where in enumerate((to_right, to_left)):
        with scope(f"w_s1_{i}"):
            hops[i].wait_recv()
        s2_out[i, i] = (sums[i] + s1_in[i].astype(F32)).astype(BF)
        copy = remote(s2_out.at[i, i], s2_in.at[i, i], s_send.at[2 + 3 * i], s_recv.at[2 + 3 * i], where)
        copy.start()
        hops.append(copy)
    own = [part(tp, 0, half), part(tp, half, half)]
    with scope("w_s2"):
        loads[3].wait()
        for copy in hops[2:]:
            copy.wait_recv()
    level = jnp.zeros((mine, 1), F32)
    streams = []
    for j in range(2):
        projected = own[j] + s2_in[0, j].astype(F32) + s2_in[1, j].astype(F32)
        stream = (resid_v[:, j * half : (j + 1) * half].astype(F32) + projected).astype(BF)
        stream_v[:, j * half : (j + 1) * half] = stream
        stream = stream.astype(F32)
        level += jnp.sum(stream * stream, axis=1, keepdims=True)
        streams.append(stream)
    factor = lax.rsqrt(level / model + 1e-06)
    for j in range(2):
        normed = (streams[j] * factor * gain_ref[:, j * half : (j + 1) * half]).astype(BF)
        packed = dot_t(chosen, normed).astype(BF)
        for b in range(NB // 2):
            at_row = (j * (NB // 2) + b) * slots
            for step in range(blocks):
                a_out[step, at_row : at_row + slots] = packed[
                    step * slots : (step + 1) * slots, b * cols : (b + 1) * cols
                ]
    forwards = []
    for step in SENDS:
        chip_at, slot = relays[step]
        for src, dst, n in ((m_out, m_in, 0), (a_out, a_in, 1)):
            copy = remote(src.at[step], dst.at[slot], a_send.at[step - 1, n], a_recv.at[slot, n], at(chip_at))
            copy.start()
            forwards.append(copy)

    line = iota((EPG * CAP * NB, 128), 0).astype(F32)
    block_of = (iota((1, 128), 1) // slots).astype(F32)

    def hits(meta):
        spots = []
        for i in range(2):
            entry = meta[i : i + 1]
            spots.append(line == jnp.where(entry > 0.0, (entry - 1.0) * NB + block_of, -1.0))
        return spots

    def send_rows(out, into, send, recv, q, turned=False):
        into[q, local] = out[q, local]

        def one(k, carry):
            other, where = peer(EPG - k if turned else k)
            remote(out.at[q, other], into.at[q, local], send.at[q], recv.at[q], where).start()
            return carry

        lax.fori_loop(1, EPG, one, 0)

    def relay(meta, tokens, q):
        one, two = hits(meta)
        sent = dot((one | two).astype(BF), tokens).astype(BF)
        b_out[q] = sent.reshape(EPG, CAP * NB, cols)
        send_rows(b_out, b_in, b_send, b_recv, q)

    def combine(meta, q):
        with scope(f"w_r{q}"):
            drain(r_in.at[q, pl.ds(0, EPG - 1)], r_recv.at[q])
        one, two = hits(meta)
        weigh = [meta[2 + 3 * i : 3 + 3 * i] + meta[3 + 3 * i : 4 + 3 * i] + meta[4 + 3 * i : 5 + 3 * i] for i in range(2)]
        weights = jnp.where(one, weigh[0], 0.0) + jnp.where(two, weigh[1], 0.0)
        high = weights.astype(BF)
        rest = (weights - high.astype(F32)).astype(BF)
        answers = r_in[q].reshape(EPG * CAP * NB, cols)
        return (dot_t(high, answers) + dot_t(rest, answers)).astype(BF)

    many = EPG * CAP
    turn_r, turn_c = iota((many * NB, many * NB), 0), iota((many * NB, many * NB), 1)
    to_blocks = (lax.rem(turn_r, many) * NB + turn_r // many == turn_c).astype(BF)
    to_rows = (lax.rem(turn_c, many) * NB + turn_c // many == turn_r).astype(BF)

    def serve(q):
        with scope(f"w_b{q}"):
            drain(b_in.at[q, pl.ds(0, EPG - 1)], b_recv.at[q])
        x = dot(to_blocks, b_in[q].reshape(many * NB, cols)).astype(BF)
        gate = jnp.zeros((many, wg_v.shape[1]), F32)
        up = jnp.zeros((many, wg_v.shape[1]), F32)
        for b in range(NB):
            xb = x[b * many : (b + 1) * many]
            gate += dot(xb, wg_v[b * cols : (b + 1) * cols])
            up += dot(xb, wu_v[b * cols : (b + 1) * cols])
        hidden = (gate * jax.nn.sigmoid(gate) * up).astype(BF)
        answers = [dot(hidden, wd_v[:, b * cols : (b + 1) * cols]).astype(BF) for b in range(NB)]
        served = dot(to_rows, jnp.concatenate(answers, axis=0)).astype(BF)
        r_out[q] = served.reshape(EPG, CAP * NB, cols)

    def answer(q):
        send_rows(r_out, r_in, r_send, r_recv, q, turned=True)

    def back(slot):
        source, step = sources[slot]
        return remote(
            c_out.at[slot],
            c_in.at[:, pl.ds(pl.multiple_of(step * slots, slots), slots)],
            c_send.at[slot],
            c_recv.at[step],
            at(source),
        )

    def store_combined(q):
        if q == 0:
            c_in[:, 0:slots] = combine(m_out[0], 0).reshape(NB, slots, cols)
        else:
            c_out[q - 1] = combine(m_in[q - 1], q).reshape(NB, slots, cols)
            back(q - 1).start()

    def pass_on(q):
        if q == 0:
            relay(m_out[0], a_out[0], 0)
        else:
            with scope(f"w_a{q}"):
                for n, ref in enumerate((m_in, a_in)):
                    drain(ref.at[q - 1], a_recv.at[q - 1, n])
            relay(m_in[q - 1], a_in[q - 1], q)

    acts = {"L": pass_on, "F": serve, "X": answer, "C": store_combined}
    for i, name in enumerate(ORDER):
        if i == 1:
            with scope("w_weights"):
                for load in loads[4:]:
                    load.wait()
        acts[name[0]](int(name[1]))

    for step in (1, 2, 3):
        with scope(f"w_c{step}"):
            drain(c_in.at[:, pl.ds(step * slots, slots)], c_recv.at[step])
    for b in range(NB):
        total = dot(chosen, c_in[b])
        span = slice(b * cols, (b + 1) * cols)
        out_ref[:, span] = (stream_v[:, span].astype(F32) + total).astype(BF)

    with scope("w_sends"):
        for copy in halo + hops + forwards:
            copy.wait_send()
        for q in range(4):
            drain(b_out.at[q, pl.ds(0, EPG - 1)], b_send.at[q])
            drain(r_out.at[q, pl.ds(0, EPG - 1)], r_send.at[q])
        for slot in range(3):
            back(slot).wait_send()


def shards(mix_in, resid_in, doc_ids, group_weight, pool_scale, out_weight, norm_gain, expert_ids, route_weights, w_gate, w_up, w_down):
    sp_size, tp_size = lax.axis_size("sp"), lax.axis_size("tp")
    rows, width = mix_in.shape
    mine, model = resid_in.shape
    hidden = w_gate.shape[2]
    cols = model // NB
    slots = mine // 2
    steps = sp_size * tp_size // EPG
    anywhere, vmem = pl.BlockSpec(memory_space=pl.ANY), pl.BlockSpec(memory_space=pltpu.VMEM)
    dma = pltpu.SemaphoreType.DMA
    message = (4, EPG, CAP * NB, cols)

    def body(*refs):
        kernel(sp_size, tp_size, *refs)

    return pl.pallas_call(
        body,
        out_shape=jax.ShapeDtypeStruct((mine, model), BF),
        in_specs=[anywhere, anywhere, vmem, anywhere, vmem, anywhere, vmem, vmem, vmem, anywhere, anywhere, anywhere],
        out_specs=vmem,
        scratch_shapes=[
            pltpu.VMEM((rows, width), BF),
            pltpu.VMEM((128, width), BF),
            pltpu.VMEM((1, rows), jnp.int32),
            pltpu.VMEM((mine, model), BF),
            pltpu.VMEM((width, width), BF),
            pltpu.VMEM((width, model), BF),
            pltpu.VMEM((model, hidden), BF),
            pltpu.VMEM((model, hidden), BF),
            pltpu.VMEM((hidden, model), BF),
            pltpu.VMEM((rows, width), BF),
            pltpu.VMEM((rows, width), BF),
            pltpu.VMEM((2, mine, model // 2), BF),
            pltpu.VMEM((2, mine, model // 2), BF),
            pltpu.VMEM((2, 2, mine, model // 2), BF),
            pltpu.VMEM((2, 2, mine, model // 2), BF),
            pltpu.VMEM((mine, model), BF),
            pltpu.VMEM((steps, NB * slots, cols), BF),
            pltpu.VMEM((steps, 8, 128), F32),
            pltpu.VMEM((steps - 1, NB * slots, cols), BF),
            pltpu.VMEM((steps - 1, 8, 128), F32),
            pltpu.VMEM(message, BF),
            pltpu.VMEM(message, BF),
            pltpu.VMEM(message, BF),
            pltpu.VMEM(message, BF),
            pltpu.VMEM((steps - 1, NB, slots, cols), BF),
            pltpu.VMEM((NB, steps * slots, cols), BF),
            dma((7,)),
            dma((4,)),
            dma((6,)),
            dma((6,)),
            dma((3, 2)),
            dma((3, 2)),
            dma((4,)),
            dma((4,)),
            dma((4,)),
            dma((4,)),
            dma((3,)),
            dma((4,)),
        ],
        compiler_params=pltpu.CompilerParams(collective_id=0, has_side_effects=True, vmem_limit_bytes=60 * 1024 * 1024),
    )(
        mix_in,
        resid_in,
        doc_ids.reshape(1, rows),
        group_weight,
        pool_scale,
        out_weight,
        norm_gain.reshape(1, model),
        expert_ids.T,
        route_weights.T,
        w_gate,
        w_up,
        w_down,
    )


def solution(mesh):
    return jax.shard_map(
        shards,
        mesh=mesh,
        in_specs=(
            P(("grp", "sp"), "tp"),
            P(("grp", "sp", "tp"), None),
            P(("grp", "sp")),
            P("tp", None, None),
            P("tp"),
            P("tp", None),
            P(),
            P(("grp", "sp", "tp"), None),
            P(("grp", "sp", "tp"), None),
            P(("sp", "tp"), None, None),
            P(("sp", "tp"), None, None),
            P(("sp", "tp"), None, None),
        ),
        out_specs=P(("grp", "sp", "tp"), None),
        check_vma=False,
    )
```
